128 devices in a mesh: sp: 16 (over z, y), tp: 8 (over x, core).
Axes of the slice: x: 4, y: 4, z: 4, core: 2. Of those that a mesh axis runs over, the one named last changes fastest.
Arguments:
- inputs: bfloat16 [16, 24576, 2048], P(None, ('sp', 'tp')), may hold values from -6 to 6
- norm_gain: bfloat16 [2048], replicated, may hold values from 0.099609375 to 1.8984375
- key_weight: bfloat16 [2048, 512], replicated, may hold values from -0.125 to 0.125
- value_weight: bfloat16 [2048, 512], replicated, may hold values from -0.125 to 0.125
- query: bfloat16 [16, 1024], P('sp', 'tp'), may hold values from -15 to 15
- head_bias: bfloat16 [16], P('tp'), may hold values from -14 to -6
Outputs:
- key_cache: bfloat16 [16, 24576, 512], P('sp', None, 'tp')
- value_cache: bfloat16 [16, 24576, 512], P('sp', None, 'tp')
- first_read: bfloat16 [16, 1024], P('sp', 'tp')
The draws below stay inside these ranges and needn't reach their ends.
All inputs are finite; a program needn't handle non-finite values.
Results may differ from the reference program's by a relative error of at most 0.012.
Values may be sent and summed in bfloat16 or wider, within the bound.
No kernel may reach another device: no remote copies, remote signals or barrier semaphores. Data moves between devices by JAX's collectives and lax.ppermute only.
A program may use at most 128 MiB of HBM per device.

```python
import math
import jax
import jax.numpy as jnp
from jax import lax

D = 2048
HEAD_DIMENSION = 64
H = 16
KVH = 8
SEQS = 16
LEN = 24576


def draw_head_bias(key, part):
    order = jax.random.permutation(jax.random.fold_in(key, 11), H)
    spread = jax.random.uniform(jax.random.fold_in(key, 12), (H,), jnp.float32)
    slow_count = H // 2
    slow_heads = order < slow_count
    lift = math.exp(3.125)
    slow_bias = jnp.log(0.5 * jnp.power(4.0, spread) / (lift * LEN))
    fast_bias = jnp.log(0.01 * jnp.power(10.0 / 3.0, spread) / lift)
    return jnp.where(slow_heads, slow_bias, fast_bias).astype(jnp.float32).astype(jnp.bfloat16)


def levels(rng, dims, cuts, smallest, largest):
    def one(position, shards_of):
        draws = jax.random.uniform(jax.random.fold_in(jax.random.fold_in(rng, 6), position), (shards_of,), jnp.float32, smallest / len(cuts), largest / len(cuts))
        return jnp.repeat(jnp.exp(draws), dims[position] // shards_of).reshape((-1,) + (1,) * (len(dims) - position - 1))

    gain = one(*cuts[0])
    for cut in cuts[1:]:
        gain = gain * one(*cut)
    return gain


def noise(own_key, shape, scale, most, shards=(), dtype=jnp.bfloat16):
    drawn = jax.random.normal(own_key, shape, jnp.float32) * scale
    if len(shards) > 0:
        drawn = levels(own_key, shape, shards, -0.22, 0.18) * drawn
    return jnp.clip(drawn, min=-most, max=most).astype(dtype)


def setup_inputs(seed: int = 0) -> dict:
    splits = jax.random.split(jax.random.key(seed), 7)
    return {
        "inputs": noise(splits[0], (SEQS, LEN, D), 1.0, 6.0, ((1, 128),)),
        "norm_gain": jnp.clip(1.0 + 0.18 * jax.random.normal(splits[1], (D,), jnp.float32), 0.099609375, 1.8984375).astype(jnp.bfloat16),
        "key_weight": noise(splits[2], (D, KVH * HEAD_DIMENSION), D ** -0.5, 0.125),
        "value_weight": noise(splits[3], (D, KVH * HEAD_DIMENSION), D ** -0.5, 0.125),
        "query": noise(splits[4], (SEQS, H * HEAD_DIMENSION), 2.5, 15.0, ((0, 16), (1, 8))),
        "head_bias": draw_head_bias(jax.random.fold_in(splits[6], 71), 0),
    }


EPSILON = 1e-06

def one_read(operands, head_bias):
    query_row, key_rows, value_rows = operands
    repeat = H // KVH
    query_tensor = query_row.astype(jnp.float32).reshape(KVH, repeat, HEAD_DIMENSION)
    key_tensor = key_rows.astype(jnp.float32).reshape(LEN, KVH, HEAD_DIMENSION)
    value_tensor = value_rows.astype(jnp.float32).reshape(LEN, KVH, HEAD_DIMENSION)
    score_logits = jnp.einsum('ebx,uex->ebu', query_tensor, key_tensor) * HEAD_DIMENSION ** (-0.5)
    score_logits = score_logits + head_bias.astype(jnp.float32).reshape(KVH, repeat, 1)
    log_keep = jax.nn.log_sigmoid(-score_logits)
    suffix_logs = lax.cumsum(log_keep, axis=2, reverse=True) - log_keep
    stick_weights = jnp.exp(jax.nn.log_sigmoid(score_logits) + suffix_logs).astype(jnp.bfloat16)
    attended_output = jnp.einsum('euq,qec->euc', stick_weights.astype(jnp.float32), value_tensor)
    return attended_output.reshape(H * HEAD_DIMENSION).astype(jnp.bfloat16)

def reference(inputs, norm_gain, key_weight, value_weight, query, head_bias):
    widened = inputs.astype(jnp.float32)
    normed = widened * lax.rsqrt(lax.optimization_barrier(jnp.mean(widened * widened, axis=-1, keepdims=True)) + EPSILON)
    normed = (normed * norm_gain.astype(jnp.float32)).astype(jnp.bfloat16)
    flat_rows = normed.reshape(-1, D)
    key_cache = jnp.dot(flat_rows, key_weight, preferred_element_type=jnp.float32).astype(jnp.bfloat16)
    value_cache = jnp.dot(flat_rows, value_weight, preferred_element_type=jnp.float32).astype(jnp.bfloat16)
    key_cache = key_cache.reshape(SEQS, LEN, KVH * HEAD_DIMENSION)
    value_cache = value_cache.reshape(SEQS, LEN, KVH * HEAD_DIMENSION)
    first_read = lax.map(lambda operands: one_read(operands, head_bias), (query, key_cache, value_cache))
    return (key_cache, value_cache, first_read)
```

```python
import jax
import jax.numpy as jnp
from jax import lax
from jax.experimental import pallas as pl
from jax.experimental.pallas import tpu as pltpu
from jax.sharding import PartitionSpec as P

HEAD_DIMENSION = 64
EPSILON = 1e-06
LANES = 128


def project_kernel(x_ref, gain_ref, key_ref, value_ref, out_ref, weight_ref, normed_ref):
    seqs, rows, width = x_ref.shape
    groups = out_ref.shape[1]

    @pl.when(pl.program_id(0) == 0)
    def _():
        half = HEAD_DIMENSION
        for pair in range(groups // 2):
            key = key_ref[:, pair * LANES : (pair + 1) * LANES]
            value = value_ref[:, pair * LANES : (pair + 1) * LANES]
            low = jnp.concatenate([key[:, :half], value[:, :half]], axis=1)
            high = jnp.concatenate([key[:, half:], value[:, half:]], axis=1)
            weight_ref[:, 2 * pair * LANES : (2 * pair + 1) * LANES] = low
            weight_ref[:, (2 * pair + 1) * LANES : (2 * pair + 2) * LANES] = high

    gain = gain_ref[...].astype(jnp.float32)
    for s in range(seqs):
        x = x_ref[s].astype(jnp.float32)
        scale = lax.rsqrt(jnp.mean(x * x, axis=-1, keepdims=True) + EPSILON)
        normed_ref[s * rows : (s + 1) * rows, :] = (x * scale * gain).astype(jnp.bfloat16)
    result = jnp.dot(normed_ref[...], weight_ref[...], preferred_element_type=jnp.float32)
    result = result.astype(jnp.bfloat16)
    for s in range(seqs):
        for g in range(groups):
            out_ref[s, g] = result[s * rows : (s + 1) * rows, g * LANES : (g + 1) * LANES]


def project(inputs, gain, key_weight, value_weight, groups, step):
    seqs, rows, width = inputs.shape
    cols = key_weight.shape[1] + value_weight.shape[1]
    return pl.pallas_call(
        project_kernel,
        grid=(seqs // step,),
        in_specs=[
            pl.BlockSpec((step, rows, width), lambda i: (i, 0, 0)),
            pl.BlockSpec((1, width), lambda i: (0, 0)),
            pl.BlockSpec(key_weight.shape, lambda i: (0, 0)),
            pl.BlockSpec(value_weight.shape, lambda i: (0, 0)),
        ],
        out_specs=pl.BlockSpec((step, groups, rows, LANES), lambda i: (i, 0, 0, 0)),
        out_shape=jax.ShapeDtypeStruct((seqs, groups, rows, LANES), jnp.bfloat16),
        scratch_shapes=[
            pltpu.VMEM((width, cols), jnp.bfloat16),
            pltpu.VMEM((step * rows, width), jnp.bfloat16),
        ],
        compiler_params=pltpu.CompilerParams(vmem_limit_bytes=56 * 1024 * 1024),
        name="project",
    )(inputs, gain.reshape(1, width), key_weight, value_weight)


def read_kernel(rows_ref, query_ref, bias_ref, key_ref, value_ref, read_ref, carry_ref, total_ref):
    step = pl.program_id(0)
    sources, span, _ = rows_ref.shape
    count = sources * span
    tiles = count // LANES

    @pl.when(step == 0)
    def _():
        carry_ref[...] = jnp.zeros_like(carry_ref)
        total_ref[...] = jnp.zeros_like(total_ref)

    half = HEAD_DIMENSION
    lane = lax.broadcasted_iota(jnp.int32, (8, LANES), 1)
    row = lax.broadcasted_iota(jnp.int32, (8, LANES), 0)
    query = jnp.broadcast_to(query_ref[...].astype(jnp.float32), (8, LANES))
    swapped = pltpu.roll(query, half, 1)
    heads = jnp.where(row == 0, query, jnp.where(row == 1, swapped, 0.0))
    heads = jnp.where(lane < half, heads, 0.0)
    eye = (
        lax.broadcasted_iota(jnp.int32, (LANES, LANES), 0)
        == lax.broadcasted_iota(jnp.int32, (LANES, LANES), 1)
    ).astype(jnp.float32)
    left = jnp.concatenate([eye, heads], axis=0).astype(jnp.bfloat16)

    block = rows_ref[...].reshape(count, LANES)
    turned = lax.dot_general(left, block, (((1,), (1,)), ((), ())), preferred_element_type=jnp.float32)
    key_ref[...] = turned[:half].astype(jnp.bfloat16)
    value_ref[...] = turned[half:LANES].astype(jnp.bfloat16)

    bias = bias_ref[...].astype(jnp.float32)
    bias = jnp.where(row == 0, bias[:, 0:1], jnp.where(row == 1, bias[:, 1:2], 0.0))
    scores = [
        turned[LANES:, n * LANES : (n + 1) * LANES] * HEAD_DIMENSION ** (-0.5) + bias for n in range(tiles)
    ]
    scores = jnp.concatenate(scores, axis=0)
    soft = jnp.log1p(jnp.exp(-jnp.abs(scores)))
    keep = jnp.minimum(-scores, 0.0) - soft
    take = jnp.minimum(scores, 0.0) - soft
    later = lax.broadcasted_iota(jnp.int32, (LANES, 2 * LANES), 0)
    here = lax.broadcasted_iota(jnp.int32, (LANES, 2 * LANES), 1)
    sums_of = jnp.where((later > here) | (here >= LANES), 1.0, 0.0)
    sums = jnp.dot(keep, sums_of, preferred_element_type=jnp.float32, precision=lax.Precision.HIGHEST)
    carry = carry_ref[...]
    suffixes = [None] * tiles
    for n in reversed(range(tiles)):
        suffixes[n] = sums[8 * n : 8 * n + 8, :LANES] + carry
        carry = carry + sums[8 * n : 8 * n + 8, LANES:]
    carry_ref[...] = carry
    weights = jnp.exp(take + jnp.concatenate(suffixes, axis=0)).astype(jnp.bfloat16)
    weights = jnp.concatenate([weights[8 * n : 8 * n + 8] for n in range(tiles)], axis=1)
    total_ref[...] += jnp.dot(weights, block, preferred_element_type=jnp.float32)

    @pl.when(step == pl.num_programs(0) - 1)
    def _():
        total = total_ref[...]
        first = pltpu.roll(total, half, 1)[0:1]
        read_ref[...] = jnp.where(lane[0:1] < half, first, total[1:2]).astype(jnp.bfloat16)


def read(received, query, bias, step):
    sources, span, _ = received.shape
    steps = sources // step
    length = sources * span
    key, value, first = pl.pallas_call(
        read_kernel,
        grid=(steps,),
        in_specs=[
            pl.BlockSpec((step, span, LANES), lambda i: (steps - 1 - i, 0, 0)),
            pl.BlockSpec((1, LANES), lambda i: (0, 0)),
            pl.BlockSpec((1, 2), lambda i: (0, 0)),
        ],
        out_specs=[
            pl.BlockSpec((HEAD_DIMENSION, step * span), lambda i: (0, steps - 1 - i)),
            pl.BlockSpec((HEAD_DIMENSION, step * span), lambda i: (0, steps - 1 - i)),
            pl.BlockSpec((1, LANES), lambda i: (0, 0)),
        ],
        out_shape=[
            jax.ShapeDtypeStruct((HEAD_DIMENSION, length), jnp.bfloat16),
            jax.ShapeDtypeStruct((HEAD_DIMENSION, length), jnp.bfloat16),
            jax.ShapeDtypeStruct((1, LANES), jnp.bfloat16),
        ],
        scratch_shapes=[pltpu.VMEM((8, LANES), jnp.float32), pltpu.VMEM((8, LANES), jnp.float32)],
        compiler_params=pltpu.CompilerParams(vmem_limit_bytes=48 * 1024 * 1024),
        name="read",
    )(received, query, bias.reshape(1, 2))
    return key.T[None], value.T[None], first


def body(inputs, norm_gain, key_weight, value_weight, query, head_bias):
    groups = lax.axis_size("tp")
    peers = lax.axis_size("sp") * groups
    span = inputs.shape[1]
    sent = project(inputs, norm_gain, key_weight, value_weight, groups, 4)
    sent = sent.reshape(peers, span, LANES)
    received = lax.all_to_all(sent, ("sp", "tp"), split_axis=0, concat_axis=0, tiled=True)
    return read(received, query, head_bias, 16)


def solution(mesh):
    placed = (P(None, ("sp", "tp"), None), P(), P(), P(), P("sp", "tp"), P("tp"))
    return jax.shard_map(
        body,
        mesh=mesh,
        in_specs=placed,
        out_specs=(P("sp", None, "tp"), P("sp", None, "tp"), P("sp", "tp")),
        check_vma=False,
    )
```

```python
import jax
import jax.numpy as jnp
from jax import lax
from jax.experimental import pallas as pl
from jax.experimental.pallas import tpu as pltpu
from jax.sharding import PartitionSpec as P

HEAD_DIMENSION = 64
EPSILON = 1e-06
LANES = 128


def project_kernel(x_ref, gain_ref, key_ref, value_ref, out_ref, normed_ref):
    seqs, rows, width = x_ref.shape
    groups = out_ref.shape[1]
    half = HEAD_DIMENSION
    odd = lax.axis_index("tp") & 1
    gain = gain_ref[...].astype(jnp.float32).reshape(1, width)

    def normalize(s, start, count, to):
        x = x_ref[s, pl.ds(start, count), :].astype(jnp.float32)
        scale = lax.rsqrt(jnp.mean(x * x, axis=-1, keepdims=True) + EPSILON)
        normed_ref[to : to + count, :] = (x * scale * gain).astype(jnp.bfloat16)

    for s in range(seqs):
        normalize(s, pl.multiple_of(odd * half, half), LANES, s * LANES)
        normalize(s, pl.multiple_of((1 - odd) * LANES, half), half, seqs * LANES + s * half)
    contract = (((0,), (1,)), ((), ()))
    keys = lax.dot_general(key_ref[...], normed_ref[...], contract, preferred_element_type=jnp.float32)
    values = lax.dot_general(value_ref[...], normed_ref[...], contract, preferred_element_type=jnp.float32)
    low = lax.broadcasted_iota(jnp.int32, (half, LANES), 1) < half
    for s in range(seqs):
        lanes = slice(s * LANES, (s + 1) * LANES)
        rest = slice((seqs + s // 2) * LANES, (seqs + s // 2 + 1) * LANES)
        for g in range(groups):
            heads = slice(g * half, (g + 1) * half)
            out_ref[s, g, :half] = keys[heads, lanes].astype(jnp.bfloat16)
            out_ref[s, g, half:LANES] = values[heads, lanes].astype(jnp.bfloat16)
            first = jnp.where(odd == 0, keys[heads, rest], values[heads, rest])
            second = jnp.where(odd == 0, values[heads, rest], keys[heads, rest])
            if s % 2 == 0:
                second = pltpu.roll(second, half, 1)
            else:
                first = pltpu.roll(first, half, 1)
            out_ref[s, g, LANES:] = jnp.where(low, first, second).astype(jnp.bfloat16)


def project(inputs, gain, key_weight, value_weight, groups, step):
    seqs, rows, width = inputs.shape
    return pl.pallas_call(
        project_kernel,
        grid=(seqs // step,),
        in_specs=[
            pl.BlockSpec((step, rows, width), lambda i: (i, 0, 0)),
            pl.BlockSpec((width,), lambda i: (0,)),
            pl.BlockSpec(key_weight.shape, lambda i: (0, 0)),
            pl.BlockSpec(value_weight.shape, lambda i: (0, 0)),
        ],
        out_specs=pl.BlockSpec((step, groups, rows, LANES), lambda i: (i, 0, 0, 0)),
        out_shape=jax.ShapeDtypeStruct((seqs, groups, rows, LANES), jnp.bfloat16),
        scratch_shapes=[pltpu.VMEM((step * rows, width), jnp.bfloat16)],
        compiler_params=pltpu.CompilerParams(vmem_limit_bytes=56 * 1024 * 1024),
        name="project",
    )(inputs, gain, key_weight, value_weight)


def read_kernel(rows_ref, query_ref, bias_ref, key_ref, value_ref, read_ref, carry_ref, total_ref):
    step = pl.program_id(0)
    sources, span, _ = rows_ref.shape
    tiles = sources * span // LANES
    half = HEAD_DIMENSION

    @pl.when(step == 0)
    def _():
        carry_ref[...] = jnp.zeros_like(carry_ref)
        total_ref[...] = jnp.zeros_like(total_ref)

    low = lax.broadcasted_iota(jnp.int32, (half, LANES), 1) < half
    for pair in range(sources // 2):
        even = rows_ref[2 * pair]
        odd = rows_ref[2 * pair + 1]
        at = 3 * LANES * pair
        key_ref[:, at : at + LANES] = even[:half]
        value_ref[:, at : at + LANES] = even[half:LANES]
        first = even[LANES:].astype(jnp.float32)
        second = odd[LANES:].astype(jnp.float32)
        key_ref[:, at + LANES : at + 2 * LANES] = jnp.where(low, first, second).astype(jnp.bfloat16)
        middle = pltpu.roll(jnp.where(low, second, first), half, 1)
        value_ref[:, at + LANES : at + 2 * LANES] = middle.astype(jnp.bfloat16)
        key_ref[:, at + 2 * LANES : at + 3 * LANES] = odd[:half]
        value_ref[:, at + 2 * LANES : at + 3 * LANES] = odd[half:LANES]

    row = lax.broadcasted_iota(jnp.int32, (8, LANES), 0)
    query = jnp.broadcast_to(query_ref[...].astype(jnp.float32), (8, LANES))
    query = jnp.where(row == 0, query, jnp.where(row == 1, pltpu.roll(query, half, 1), 0.0))
    query = query[:, :half].astype(jnp.bfloat16)
    logits = jnp.dot(query, key_ref[...], preferred_element_type=jnp.float32)
    bias = bias_ref[...].astype(jnp.float32)
    bias = jnp.where(row == 0, bias[:, 0:1], jnp.where(row == 1, bias[:, 1:2], 0.0))
    scores = [logits[:, n * LANES : (n + 1) * LANES] * HEAD_DIMENSION ** (-0.5) + bias for n in range(tiles)]
    scores = jnp.concatenate(scores, axis=0)
    soft = jnp.log1p(jnp.exp(-jnp.abs(scores)))
    keep = jnp.minimum(-scores, 0.0) - soft
    take = jnp.minimum(scores, 0.0) - soft
    later = lax.broadcasted_iota(jnp.int32, (LANES, 2 * LANES), 0)
    here = lax.broadcasted_iota(jnp.int32, (LANES, 2 * LANES), 1)
    sums_of = jnp.where((later > here) | (here >= LANES), 1.0, 0.0)
    sums = jnp.dot(keep, sums_of, preferred_element_type=jnp.float32, precision=lax.Precision.HIGHEST)
    carry = carry_ref[...]
    suffixes = [None] * tiles
    for n in reversed(range(tiles)):
        suffixes[n] = sums[8 * n : 8 * n + 8, :LANES] + carry
        carry = carry + sums[8 * n : 8 * n + 8, LANES:]
    carry_ref[...] = carry
    weights = jnp.exp(take + jnp.concatenate(suffixes, axis=0)).astype(jnp.bfloat16)
    weights = jnp.concatenate([weights[8 * n : 8 * n + 8] for n in range(tiles)], axis=1)
    total_ref[...] += lax.dot_general(
        weights, value_ref[...], (((1,), (1,)), ((), ())), preferred_element_type=jnp.float32
    )

    @pl.when(step == pl.num_programs(0) - 1)
    def _():
        read_ref[:, :half] = total_ref[0:1].astype(jnp.bfloat16)
        read_ref[:, half:] = total_ref[1:2].astype(jnp.bfloat16)


def read(received, query, bias, step):
    sources, span, _ = received.shape
    steps = sources // step
    length = sources * span
    key, value, first = pl.pallas_call(
        read_kernel,
        grid=(steps,),
        in_specs=[
            pl.BlockSpec((step, span, LANES), lambda i: (steps - 1 - i, 0, 0)),
            pl.BlockSpec((1, LANES), lambda i: (0, 0)),
            pl.BlockSpec((1, 2), lambda i: (0, 0)),
        ],
        out_specs=[
            pl.BlockSpec((HEAD_DIMENSION, step * span), lambda i: (0, steps - 1 - i)),
            pl.BlockSpec((HEAD_DIMENSION, step * span), lambda i: (0, steps - 1 - i)),
            pl.BlockSpec((1, LANES), lambda i: (0, 0)),
        ],
        out_shape=[
            jax.ShapeDtypeStruct((HEAD_DIMENSION, length), jnp.bfloat16),
            jax.ShapeDtypeStruct((HEAD_DIMENSION, length), jnp.bfloat16),
            jax.ShapeDtypeStruct((1, LANES), jnp.bfloat16),
        ],
        scratch_shapes=[pltpu.VMEM((8, LANES), jnp.float32), pltpu.VMEM((8, HEAD_DIMENSION), jnp.float32)],
        compiler_params=pltpu.CompilerParams(vmem_limit_bytes=24 * 1024 * 1024),
        name="read",
    )(received, query, bias.reshape(1, 2))
    return key.T[None], value.T[None], first


def body(inputs, norm_gain, key_weight, value_weight, query, head_bias):
    groups = lax.axis_size("tp")
    peers = lax.axis_size("sp") * groups
    span = inputs.shape[1]
    sent = project(inputs, norm_gain, key_weight, value_weight, groups, 4)
    sent = sent.reshape(peers, span, LANES)
    received = lax.all_to_all(sent, ("sp", "tp"), split_axis=0, concat_axis=0, tiled=True)
    return read(received, query, head_bias, 32)


def solution(mesh):
    placed = (P(None, ("sp", "tp"), None), P(), P(), P(), P("sp", "tp"), P("tp"))
    return jax.shard_map(
        body,
        mesh=mesh,
        in_specs=placed,
        out_specs=(P("sp", None, "tp"), P("sp", None, "tp"), P("sp", "tp")),
        check_vma=False,
    )
```

```python
import jax
import jax.numpy as jnp
from jax import lax
from jax.experimental import pallas as pl
from jax.experimental.pallas import tpu as pltpu
from jax.sharding import PartitionSpec as P

HEAD_DIMENSION = 64
EPSILON = 1e-06
LANES = 128


def project_kernel(x_ref, gain_ref, key_ref, value_ref, out_ref, normed_ref):
    seqs, rows, width = x_ref.shape
    groups = out_ref.shape[1]
    half = HEAD_DIMENSION
    odd = lax.axis_index("tp") & 1
    gain = gain_ref[...].astype(jnp.float32).reshape(1, width)

    def normalize(s, start, count, to):
        x = x_ref[s, pl.ds(start, count), :].astype(jnp.float32)
        scale = lax.rsqrt(jnp.mean(x * x, axis=-1, keepdims=True) + EPSILON)
        normed_ref[to : to + count, :] = (x * scale * gain).astype(jnp.bfloat16)

    for s in range(seqs):
        normalize(s, pl.multiple_of(odd * half, half), LANES, s * LANES)
    for s in range(seqs):
        normalize(s, pl.multiple_of((1 - odd) * LANES, half), half, seqs * LANES + s * half)
    contract = (((0,), (1,)), ((), ()))
    keys = lax.dot_general(key_ref[...], normed_ref[...], contract, preferred_element_type=jnp.float32)
    values = lax.dot_general(value_ref[...], normed_ref[...], contract, preferred_element_type=jnp.float32)
    low = lax.broadcasted_iota(jnp.int32, (half, LANES), 1) < half
    for s in range(seqs):
        lanes = slice(s * LANES, (s + 1) * LANES)
        rest = slice((seqs + s // 2) * LANES, (seqs + s // 2 + 1) * LANES)
        for g in range(groups):
            heads = slice(g * half, (g + 1) * half)
            out_ref[s, g, :half] = keys[heads, lanes].astype(jnp.bfloat16)
            out_ref[s, g, half:LANES] = values[heads, lanes].astype(jnp.bfloat16)
            first = jnp.where(odd == 0, keys[heads, rest], values[heads, rest])
            second = jnp.where(odd == 0, values[heads, rest], keys[heads, rest])
            if s % 2 == 0:
                second = pltpu.roll(second, half, 1)
            else:
                first = pltpu.roll(first, half, 1)
            out_ref[s, g, LANES:] = jnp.where(low, first, second).astype(jnp.bfloat16)


def project(inputs, gain, key_weight, value_weight, groups, step):
    seqs, rows, width = inputs.shape
    return pl.pallas_call(
        project_kernel,
        grid=(seqs // step,),
        in_specs=[
            pl.BlockSpec((step, rows, width), lambda i: (i, 0, 0)),
            pl.BlockSpec((width,), lambda i: (0,)),
            pl.BlockSpec(key_weight.shape, lambda i: (0, 0)),
            pl.BlockSpec(value_weight.shape, lambda i: (0, 0)),
        ],
        out_specs=pl.BlockSpec((step, groups, rows, LANES), lambda i: (i, 0, 0, 0)),
        out_shape=jax.ShapeDtypeStruct((seqs, groups, rows, LANES), jnp.bfloat16),
        scratch_shapes=[pltpu.VMEM((step * rows, width), jnp.bfloat16)],
        compiler_params=pltpu.CompilerParams(vmem_limit_bytes=56 * 1024 * 1024),
        name="project",
    )(inputs, gain, key_weight, value_weight)


def read_kernel(rows_ref, query_ref, bias_ref, key_ref, value_ref, read_ref, carry_ref, total_ref):
    step = pl.program_id(0)
    sources, span, _ = rows_ref.shape
    tiles = sources * span // LANES
    half = HEAD_DIMENSION

    @pl.when(step == 0)
    def _():
        carry_ref[...] = jnp.zeros_like(carry_ref)
        total_ref[...] = jnp.zeros_like(total_ref)

    low = lax.broadcasted_iota(jnp.int32, (half, LANES), 1) < half
    for pair in range(sources // 2):
        even = rows_ref[2 * pair]
        odd = rows_ref[2 * pair + 1]
        at = 3 * LANES * pair
        key_ref[:, at : at + LANES] = even[:half]
        value_ref[:, at : at + LANES] = even[half:LANES]
        first = even[LANES:].astype(jnp.float32)
        second = odd[LANES:].astype(jnp.float32)
        key_ref[:, at + LANES : at + 2 * LANES] = jnp.where(low, first, second).astype(jnp.bfloat16)
        middle = pltpu.roll(jnp.where(low, second, first), half, 1)
        value_ref[:, at + LANES : at + 2 * LANES] = middle.astype(jnp.bfloat16)
        key_ref[:, at + 2 * LANES : at + 3 * LANES] = odd[:half]
        value_ref[:, at + 2 * LANES : at + 3 * LANES] = odd[half:LANES]

    row = lax.broadcasted_iota(jnp.int32, (8, LANES), 0)
    query = jnp.broadcast_to(query_ref[...].astype(jnp.float32), (8, LANES))
    query = jnp.where(row == 0, query, jnp.where(row == 1, pltpu.roll(query, half, 1), 0.0))
    query = query[:, :half].astype(jnp.bfloat16)
    logits = jnp.dot(query, key_ref[...], preferred_element_type=jnp.float32)
    bias = bias_ref[...].astype(jnp.float32)
    bias = jnp.where(row == 0, bias[:, 0:1], jnp.where(row == 1, bias[:, 1:2], 0.0))
    scores = [logits[:, n * LANES : (n + 1) * LANES] * HEAD_DIMENSION ** (-0.5) + bias for n in range(tiles)]
    scores = jnp.concatenate(scores, axis=0)
    soft = jnp.log1p(jnp.exp(-jnp.abs(scores)))
    keep = jnp.minimum(-scores, 0.0) - soft
    take = jnp.minimum(scores, 0.0) - soft
    later = lax.broadcasted_iota(jnp.int32, (LANES, 2 * LANES), 0)
    here = lax.broadcasted_iota(jnp.int32, (LANES, 2 * LANES), 1)
    sums_of = jnp.where((later > here) | (here >= LANES), 1.0, 0.0)
    sums_of = sums_of.astype(jnp.bfloat16)
    pieces = []
    for _ in range(3):
        pieces.append(keep.astype(jnp.bfloat16))
        keep = keep - pieces[-1].astype(jnp.float32)
    sums = jnp.dot(
        jnp.concatenate(pieces, axis=1),
        jnp.concatenate([sums_of] * 3, axis=0),
        preferred_element_type=jnp.float32,
    )
    carry = carry_ref[...]
    suffixes = [None] * tiles
    for top in reversed(range(0, tiles, 8)):
        later_tiles = None
        for n in reversed(range(top, top + 8)):
            own = sums[8 * n : 8 * n + 8, :LANES]
            suffixes[n] = own if later_tiles is None else own + later_tiles
            whole = sums[8 * n : 8 * n + 8, LANES:]
            later_tiles = whole if later_tiles is None else later_tiles + whole
        for n in range(top, top + 8):
            suffixes[n] = suffixes[n] + carry
        carry = carry + later_tiles
    carry_ref[...] = carry
    weights = jnp.exp(take + jnp.concatenate(suffixes, axis=0)).astype(jnp.bfloat16)
    weights = jnp.concatenate([weights[8 * n : 8 * n + 8] for n in range(tiles)], axis=1)
    total_ref[...] += lax.dot_general(
        weights, value_ref[...], (((1,), (1,)), ((), ())), preferred_element_type=jnp.float32
    )

    @pl.when(step == pl.num_programs(0) - 1)
    def _():
        read_ref[:, :half] = total_ref[0:1].astype(jnp.bfloat16)
        read_ref[:, half:] = total_ref[1:2].astype(jnp.bfloat16)


def read(received, query, bias, step):
    sources, span, _ = received.shape
    steps = sources // step
    length = sources * span
    key, value, first = pl.pallas_call(
        read_kernel,
        grid=(steps,),
        in_specs=[
            pl.BlockSpec((step, span, LANES), lambda i: (steps - 1 - i, 0, 0)),
            pl.BlockSpec((1, LANES), lambda i: (0, 0)),
            pl.BlockSpec((1, 2), lambda i: (0, 0)),
        ],
        out_specs=[
            pl.BlockSpec((HEAD_DIMENSION, step * span), lambda i: (0, steps - 1 - i)),
            pl.BlockSpec((HEAD_DIMENSION, step * span), lambda i: (0, steps - 1 - i)),
            pl.BlockSpec((1, LANES), lambda i: (0, 0)),
        ],
        out_shape=[
            jax.ShapeDtypeStruct((HEAD_DIMENSION, length), jnp.bfloat16),
            jax.ShapeDtypeStruct((HEAD_DIMENSION, length), jnp.bfloat16),
            jax.ShapeDtypeStruct((1, LANES), jnp.bfloat16),
        ],
        scratch_shapes=[pltpu.VMEM((8, LANES), jnp.float32), pltpu.VMEM((8, HEAD_DIMENSION), jnp.float32)],
        compiler_params=pltpu.CompilerParams(vmem_limit_bytes=36 * 1024 * 1024),
        name="read",
    )(received, query, bias.reshape(1, 2))
    return key.T[None], value.T[None], first


def body(inputs, norm_gain, key_weight, value_weight, query, head_bias):
    groups = lax.axis_size("tp")
    peers = lax.axis_size("sp") * groups
    span = inputs.shape[1]
    sent = project(inputs, norm_gain, key_weight, value_weight, groups, 4)
    sent = sent.reshape(peers, span, LANES)
    received = lax.all_to_all(sent, ("sp", "tp"), split_axis=0, concat_axis=0, tiled=True)
    return read(received, query, head_bias, 64)


def solution(mesh):
    placed = (P(None, ("sp", "tp"), None), P(), P(), P(), P("sp", "tp"), P("tp"))
    return jax.shard_map(
        body,
        mesh=mesh,
        in_specs=placed,
        out_specs=(P("sp", None, "tp"), P("sp", None, "tp"), P("sp", "tp")),
        check_vma=False,
    )
```

```python
import jax
import jax.numpy as jnp
from jax import lax
from jax.experimental import pallas as pl
from jax.experimental.pallas import tpu as pltpu
from jax.sharding import PartitionSpec as P

HEAD_DIMENSION = 64
EPSILON = 1e-06
LANES = 128


def project_kernel(x_ref, gain_ref, key_ref, value_ref, out_ref, normed_ref):
    seqs, rows, width = x_ref.shape
    groups = out_ref.shape[1]
    half = HEAD_DIMENSION
    odd = lax.axis_index("tp") & 1
    gain = gain_ref[...].astype(jnp.float32).reshape(1, width)

    def normalize(s, start, count, to):
        x = x_ref[s, pl.ds(start, count), :].astype(jnp.float32)
        scale = lax.rsqrt(jnp.mean(x * x, axis=-1, keepdims=True) + EPSILON)
        normed_ref[to : to + count, :] = (x * scale * gain).astype(jnp.bfloat16)

    for s in range(seqs):
        normalize(s, pl.multiple_of(odd * half, half), LANES, s * LANES)
    for s in range(seqs):
        normalize(s, pl.multiple_of((1 - odd) * LANES, half), half, seqs * LANES + s * half)
    contract = (((0,), (1,)), ((), ()))
    keys = lax.dot_general(key_ref[...], normed_ref[...], contract, preferred_element_type=jnp.float32)
    values = lax.dot_general(value_ref[...], normed_ref[...], contract, preferred_element_type=jnp.float32)
    low = lax.broadcasted_iota(jnp.int32, (half, LANES), 1) < half
    for s in range(seqs):
        lanes = slice(s * LANES, (s + 1) * LANES)
        rest = slice((seqs + s // 2) * LANES, (seqs + s // 2 + 1) * LANES)
        for g in range(groups):
            heads = slice(g * half, (g + 1) * half)
            out_ref[s, g, :half] = keys[heads, lanes].astype(jnp.bfloat16)
            out_ref[s, g, half:LANES] = values[heads, lanes].astype(jnp.bfloat16)
            first = jnp.where(odd == 0, keys[heads, rest], values[heads, rest])
            second = jnp.where(odd == 0, values[heads, rest], keys[heads, rest])
            if s % 2 == 0:
                second = pltpu.roll(second, half, 1)
            else:
                first = pltpu.roll(first, half, 1)
            out_ref[s, g, LANES:] = jnp.where(low, first, second).astype(jnp.bfloat16)


def project(inputs, gain, key_weight, value_weight, groups, step):
    seqs, rows, width = inputs.shape
    return pl.pallas_call(
        project_kernel,
        grid=(seqs // step,),
        in_specs=[
            pl.BlockSpec((step, rows, width), lambda i: (i, 0, 0)),
            pl.BlockSpec((width,), lambda i: (0,)),
            pl.BlockSpec(key_weight.shape, lambda i: (0, 0)),
            pl.BlockSpec(value_weight.shape, lambda i: (0, 0)),
        ],
        out_specs=pl.BlockSpec((step, groups, rows, LANES), lambda i: (i, 0, 0, 0)),
        out_shape=jax.ShapeDtypeStruct((seqs, groups, rows, LANES), jnp.bfloat16),
        scratch_shapes=[pltpu.VMEM((step * rows, width), jnp.bfloat16)],
        compiler_params=pltpu.CompilerParams(vmem_limit_bytes=56 * 1024 * 1024),
        name="project",
    )(inputs, gain, key_weight, value_weight)


def read_kernel(rows_ref, query_ref, bias_ref, key_ref, value_ref, read_ref, carry_ref, total_ref):
    step = pl.program_id(0)
    sources, span, _ = rows_ref.shape
    tiles = sources * span // LANES
    half = HEAD_DIMENSION

    @pl.when(step == 0)
    def _():
        carry_ref[...] = jnp.zeros_like(carry_ref)
        total_ref[...] = jnp.zeros_like(total_ref)

    low = lax.broadcasted_iota(jnp.int32, (half, LANES), 1) < half
    for pair in range(sources // 2):
        even = rows_ref[2 * pair]
        odd = rows_ref[2 * pair + 1]
        at = 3 * LANES * pair
        key_ref[:, at : at + LANES] = even[:half]
        value_ref[:, at : at + LANES] = even[half:LANES]
        first = even[LANES:]
        second = odd[LANES:]
        key_ref[:, at + LANES : at + 2 * LANES] = jnp.where(low, first, second)
        middle = pltpu.roll(jnp.where(low, second, first).astype(jnp.float32), half, 1)
        value_ref[:, at + LANES : at + 2 * LANES] = middle.astype(jnp.bfloat16)
        key_ref[:, at + 2 * LANES : at + 3 * LANES] = odd[:half]
        value_ref[:, at + 2 * LANES : at + 3 * LANES] = odd[half:LANES]

    row = lax.broadcasted_iota(jnp.int32, (8, LANES), 0)
    query = jnp.broadcast_to(query_ref[...].astype(jnp.float32), (8, LANES))
    query = jnp.where(row == 0, query, jnp.where(row == 1, pltpu.roll(query, half, 1), 0.0))
    query = query[:, :half].astype(jnp.bfloat16)
    logits = jnp.dot(query, key_ref[...], preferred_element_type=jnp.float32)
    bias = bias_ref[...].astype(jnp.float32)
    bias = jnp.where(row == 0, bias[:, 0:1], jnp.where(row == 1, bias[:, 1:2], 0.0))
    scores = [logits[:, n * LANES : (n + 1) * LANES] * HEAD_DIMENSION ** (-0.5) + bias for n in range(tiles)]
    scores = jnp.concatenate(scores, axis=0)
    soft = jnp.log1p(jnp.exp(-jnp.abs(scores)))
    keep = jnp.minimum(-scores, 0.0) - soft
    take = jnp.minimum(scores, 0.0) - soft
    later = lax.broadcasted_iota(jnp.int32, (LANES, 2 * LANES), 0)
    here = lax.broadcasted_iota(jnp.int32, (LANES, 2 * LANES), 1)
    sums_of = jnp.where((later > here) | (here >= LANES), 1.0, 0.0)
    sums_of = sums_of.astype(jnp.bfloat16)
    pieces = []
    for _ in range(3):
        pieces.append(keep.astype(jnp.bfloat16))
        keep = keep - pieces[-1].astype(jnp.float32)
    sums = jnp.dot(
        jnp.concatenate(pieces, axis=1),
        jnp.concatenate([sums_of] * 3, axis=0),
        preferred_element_type=jnp.float32,
    )
    carry = carry_ref[...]
    suffixes = [None] * tiles
    for top in reversed(range(0, tiles, 8)):
        later_tiles = None
        for n in reversed(range(top, top + 8)):
            own = sums[8 * n : 8 * n + 8, :LANES]
            suffixes[n] = own if later_tiles is None else own + later_tiles
            whole = sums[8 * n : 8 * n + 8, LANES:]
            later_tiles = whole if later_tiles is None else later_tiles + whole
        for n in range(top, top + 8):
            suffixes[n] = suffixes[n] + carry
        carry = carry + later_tiles
    carry_ref[...] = carry
    weights = jnp.exp(take + jnp.concatenate(suffixes, axis=0)).astype(jnp.bfloat16)
    weights = jnp.concatenate([weights[8 * n : 8 * n + 8] for n in range(tiles)], axis=1)
    total_ref[...] += lax.dot_general(
        weights, value_ref[...], (((1,), (1,)), ((), ())), preferred_element_type=jnp.float32
    )

    @pl.when(step == pl.num_programs(0) - 1)
    def _():
        read_ref[:, :half] = total_ref[0:1].astype(jnp.bfloat16)
        read_ref[:, half:] = total_ref[1:2].astype(jnp.bfloat16)


def read(received, query, bias, step):
    sources, span, _ = received.shape
    steps = sources // step
    length = sources * span
    key, value, first = pl.pallas_call(
        read_kernel,
        grid=(steps,),
        in_specs=[
            pl.BlockSpec((step, span, LANES), lambda i: (steps - 1 - i, 0, 0)),
            pl.BlockSpec((1, LANES), lambda i: (0, 0)),
            pl.BlockSpec((1, 2), lambda i: (0, 0)),
        ],
        out_specs=[
            pl.BlockSpec((HEAD_DIMENSION, step * span), lambda i: (0, steps - 1 - i)),
            pl.BlockSpec((HEAD_DIMENSION, step * span), lambda i: (0, steps - 1 - i)),
            pl.BlockSpec((1, LANES), lambda i: (0, 0)),
        ],
        out_shape=[
            jax.ShapeDtypeStruct((HEAD_DIMENSION, length), jnp.bfloat16),
            jax.ShapeDtypeStruct((HEAD_DIMENSION, length), jnp.bfloat16),
            jax.ShapeDtypeStruct((1, LANES), jnp.bfloat16),
        ],
        scratch_shapes=[pltpu.VMEM((8, LANES), jnp.float32), pltpu.VMEM((8, HEAD_DIMENSION), jnp.float32)],
        compiler_params=pltpu.CompilerParams(vmem_limit_bytes=36 * 1024 * 1024),
        name="read",
    )(received, query, bias.reshape(1, 2))
    return key.T[None], value.T[None], first


def body(inputs, norm_gain, key_weight, value_weight, query, head_bias):
    groups = lax.axis_size("tp")
    peers = lax.axis_size("sp") * groups
    span = inputs.shape[1]
    sent = project(inputs, norm_gain, key_weight, value_weight, groups, 4)
    sent = sent.reshape(peers, span, LANES)
    received = lax.all_to_all(sent, ("sp", "tp"), split_axis=0, concat_axis=0, tiled=True)
    return read(received, query, head_bias, 64)


def solution(mesh):
    placed = (P(None, ("sp", "tp"), None), P(), P(), P(), P("sp", "tp"), P("tp"))
    return jax.shard_map(
        body,
        mesh=mesh,
        in_specs=placed,
        out_specs=(P("sp", None, "tp"), P("sp", None, "tp"), P("sp", "tp")),
        check_vma=False,
    )
```
